1024 devices in a mesh: sp: 128 (over z, y), tp: 8 (over x, core).
Axes of the slice: x: 4, y: 4, z: 32, core: 2. Of those that a mesh axis runs over, the one named last changes fastest.
Arguments:
- query_rows: bfloat16 [32768, 2048], P('sp', 'tp'), may hold values from -5.5 to 5.5
- key_rows: bfloat16 [32768, 2048], P('sp', 'tp'), may hold values from -5.5 to 5.5
- value_rows: bfloat16 [32768, 2048], P('sp', 'tp'), may hold values from -6 to 6
- out_grad: bfloat16 [32768, 2048], P('sp', 'tp'), may hold values from -96 to 96
- rel_bias: float32 [256, 32], replicated, may hold values from -3 to 3
Outputs:
- query_grad: bfloat16 [32768, 2048], P('sp', 'tp')
- key_grad: bfloat16 [32768, 2048], P('sp', 'tp')
- value_grad: bfloat16 [32768, 2048], P('sp', 'tp')
- table_grad: float32 [256, 32], P('sp')
The draws below stay inside these ranges and needn't reach their ends.
All inputs are finite; a program needn't handle non-finite values.
Results may differ from the reference program's by a relative error of at most 0.007.
Values may be sent and summed in bfloat16 or wider, within the bound.
No kernel may reach another device: no remote copies, remote signals or barrier semaphores. Data moves between devices by JAX's collectives and lax.ppermute only.
A program may use at most 32 MiB of HBM per device.

```python
import jax
import jax.numpy as jnp
from jax import lax

HEADS = 32
HEAD_DIM = 64
SEG = 64
LEFT = 4
CLIP = 128
TOKENS = 32768
TABLE = 256


def drawn_pair(key):
    key_queries, key_keys = jax.random.split(jax.random.fold_in(key, 11), 2)
    width_all = HEADS * HEAD_DIM
    query_draw = jnp.clip(jax.random.normal(key_queries, (TOKENS, width_all), jnp.float32), -5.5, 5.5)
    key_draw = jnp.clip(jax.random.normal(key_keys, (TOKENS, width_all), jnp.float32), -5.5, 5.5)
    return (query_draw, key_draw)


def draw_query_rows(key, part):
    return drawn_pair(key)[0].astype(jnp.bfloat16)


def draw_key_rows(key, part):
    return drawn_pair(key)[1].astype(jnp.bfloat16)


def steps_of(rng, shape, shards, low, top_value):
    def one(dim, shards_of):
        draws = jax.random.uniform(jax.random.fold_in(jax.random.fold_in(rng, 6), dim), (shards_of,), jnp.float32, low / len(shards), top_value / len(shards))
        return jnp.repeat(jnp.exp(draws), shape[dim] // shards_of).reshape((-1,) + (1,) * (len(shape) - dim - 1))

    loudness = one(*shards[0])
    for cut in shards[1:]:
        loudness = loudness * one(*cut)
    return loudness


def gaussian(rng, dims, width, limit, pieces=(), kind=jnp.bfloat16):
    factor_of = steps_of(rng, dims, pieces, -0.22, 0.18) if pieces else 1.0
    drawn = jax.random.normal(rng, dims, jnp.float32) * width * factor_of
    return jnp.minimum(jnp.maximum(drawn, -limit), limit).astype(kind)


def setup_inputs(seed: int = 0) -> dict:
    key_of = jax.random.split(jax.random.key(seed), 6)
    return {
        "query_rows": draw_query_rows(jax.random.fold_in(key_of[5], 71), 0),
        "key_rows": draw_key_rows(jax.random.fold_in(key_of[5], 71), 0),
        "value_rows": gaussian(key_of[2], (TOKENS, HEADS * HEAD_DIM), 1.0, 6.0, ((0, 128), (1, 8))),
        "out_grad": gaussian(key_of[3], (TOKENS, HEADS * HEAD_DIM), 16.0, 96.0, ((0, 128), (1, 8))),
        "rel_bias": gaussian(key_of[4], (TABLE, HEADS), 0.5, 3.0, (), jnp.float32),
    }


NEG_FILL = -1e30


def banded(extended, seg_count, seg_len, band_len):
    layers = []
    for offset in range(band_len // seg_len):
        window = lax.slice_in_dim(extended, offset * seg_len, offset * seg_len + seg_count * seg_len, axis=0)
        layers.append(window.reshape((seg_count, 1, seg_len) + extended.shape[1:]))
    return jnp.concatenate(layers, axis=1).reshape((seg_count, band_len) + extended.shape[1:])


def unbanded(band_grads, ext_len, seg_len):
    seg_count, band_len = band_grads.shape[0], band_grads.shape[1]
    trailing = band_grads.shape[2:]
    blocks = band_grads.reshape((seg_count, band_len // seg_len, seg_len) + trailing)
    summed = jnp.zeros((ext_len,) + trailing, band_grads.dtype)
    for offset in range(band_len // seg_len):
        stripe = blocks[:, offset].reshape((seg_count * seg_len,) + trailing)
        widths = [(offset * seg_len, ext_len - offset * seg_len - seg_count * seg_len)] + [(0, 0)] * len(trailing)
        summed = summed + jnp.pad(stripe, widths)
    return summed


def head_backward(inputs):
    query_head, key_head, value_head, dout_head, table_col = inputs
    reach_rows = LEFT * SEG
    band_len = reach_rows + SEG
    seg_count = TOKENS // SEG
    score_scale = HEAD_DIM ** -0.5
    key_ext = jnp.pad(key_head.astype(jnp.float32), ((reach_rows, 0), (0, 0)))
    value_ext = jnp.pad(value_head.astype(jnp.float32), ((reach_rows, 0), (0, 0)))
    key_valid = jnp.arange(reach_rows + TOKENS, dtype=jnp.int32) >= reach_rows
    key_band = banded(key_ext, seg_count, SEG, band_len)
    value_band = banded(value_ext, seg_count, SEG, band_len)
    valid_band = banded(key_valid, seg_count, SEG, band_len)
    query_segs = query_head.astype(jnp.float32).reshape(seg_count, SEG, HEAD_DIM)
    dout_segs = dout_head.astype(jnp.float32).reshape(seg_count, SEG, HEAD_DIM)
    row_pos = jnp.arange(SEG, dtype=jnp.int32)[:, None]
    col_pos = jnp.arange(band_len, dtype=jnp.int32)[None, :]
    offset_index = jnp.clip(reach_rows + row_pos - col_pos, -CLIP, CLIP - 1) + CLIP
    bias_band = table_col[offset_index]
    scores = jnp.einsum('jid,jcd->jic', query_segs, key_band) * score_scale + bias_band[None]
    scores = jnp.where(valid_band[:, None, :], scores, NEG_FILL)
    row_peak = jnp.max(scores, axis=-1)
    log_norm = row_peak + jnp.log(jnp.sum(jnp.exp(scores - row_peak[..., None]), axis=-1))
    attention = jnp.exp(scores - log_norm[..., None])
    attention_half = lax.optimization_barrier(attention.astype(jnp.bfloat16)).astype(jnp.float32)
    attention_grad = jnp.einsum('jie,jce->jic', dout_segs, value_band)
    inner_sums = jnp.sum(attention * attention_grad, axis=-1)
    dscores = attention * (attention_grad - inner_sums[..., None])
    dscore_half = lax.optimization_barrier(dscores.astype(jnp.bfloat16)).astype(jnp.float32)
    dquery = (jnp.einsum('jic,jcd->jid', dscore_half, key_band) * score_scale).reshape(TOKENS, HEAD_DIM)
    dkey_band = jnp.einsum('jic,jid->jcd', dscore_half, query_segs) * score_scale
    dvalue_band = jnp.einsum('jic,jie->jce', attention_half, dout_segs)
    key_grad_rows = unbanded(dkey_band, reach_rows + TOKENS, SEG)[reach_rows:]
    value_grad_rows = unbanded(dvalue_band, reach_rows + TOKENS, SEG)[reach_rows:]
    table_col_grad = jax.ops.segment_sum(jnp.sum(dscores, axis=0).reshape(-1), offset_index.reshape(-1), num_segments=2 * CLIP)
    return dquery.astype(jnp.bfloat16), key_grad_rows.astype(jnp.bfloat16), value_grad_rows.astype(jnp.bfloat16), table_col_grad


def split_heads(row_block):
    return jnp.transpose(row_block.reshape(TOKENS, HEADS, HEAD_DIM), (1, 0, 2))


def join_heads(stacked):
    return jnp.transpose(stacked, (1, 0, 2)).reshape(TOKENS, HEADS * HEAD_DIM)


def reference(query_rows, key_rows, value_rows, out_grad, rel_bias):
    results = lax.map(head_backward, (split_heads(query_rows), split_heads(key_rows), split_heads(value_rows), split_heads(out_grad), jnp.transpose(rel_bias)))
    return (join_heads(results[0]), join_heads(results[1]), join_heads(results[2]), jnp.transpose(results[3]))
```

```python
from functools import partial

import jax
import jax.numpy as jnp
from jax import lax
from jax.experimental import pallas as pl
from jax.experimental.pallas import tpu as pltpu
from jax.sharding import PartitionSpec as P

HEAD_DIM = 64
SEG = 64
LEFT = 4
CLIP = 128
NEG_FILL = -1e30
HIGHEST = lax.Precision.HIGHEST

REACH = LEFT * SEG
PAIR = 2 * SEG
WIN = REACH + PAIR

NT = (((1,), (1,)), ((), ()))
TN = (((0,), (0,)), ((), ()))
NN = (((1,), (0,)), ((), ()))


def dot(a, b, dims, **kw):
    return lax.dot_general(a, b, dims, preferred_element_type=jnp.float32, **kw)


def bias_kernel(first_head, table_ref, bias_ref):
    heads = bias_ref.shape[1] // PAIR
    wide = table_ref.shape[1]
    start = first_head(heads)
    pick = lax.broadcasted_iota(jnp.int32, (8, wide), 1) == lax.broadcasted_iota(jnp.int32, (8, wide), 0) + start
    rows = dot(jnp.where(pick, 1.0, 0.0), table_ref[...], NT, precision=HIGHEST)
    key_of = lax.broadcasted_iota(jnp.int32, (PAIR, PAIR), 0)
    query_of = lax.broadcasted_iota(jnp.int32, (PAIR, PAIR), 1)
    early = query_of < SEG
    low = key_of < SEG
    after = query_of >= key_of
    for head in range(heads):
        lanes = slice(head * PAIR, (head + 1) * PAIR)
        neg = jnp.broadcast_to(rows[head : head + 1, :CLIP], (PAIR, PAIR))
        pos = jnp.broadcast_to(rows[head : head + 1, CLIP:], (PAIR, PAIR))
        neg = pltpu.roll(neg, 0, 1, stride=1, stride_axis=0)
        pos = pltpu.roll(pos, 0, 1, stride=1, stride_axis=0)
        top = rows[head : head + 1, 2 * CLIP - 1 :]
        bias_ref[0:PAIR, lanes] = jnp.where(low & ~early, NEG_FILL, jnp.broadcast_to(top, (PAIR, PAIR)))
        bias_ref[PAIR : 2 * PAIR, lanes] = jnp.where(after, top, pos)
        bias_ref[2 * PAIR : 3 * PAIR, lanes] = jnp.where(early & ~low, NEG_FILL, jnp.where(after, pos, neg))


def diagonals(squares):
    rows = PAIR
    while rows > 8:
        half = rows // 2
        squares = [s[:half] + pltpu.roll(s[half:], PAIR - half, 1) for s in squares]
        rows = half
    row_of = lax.broadcasted_iota(jnp.int32, (8, PAIR), 0)
    sums = []
    for s in squares:
        for bit in (4, 2, 1):
            s = jnp.where((row_of & bit) != 0, pltpu.roll(s, PAIR - bit, 1), s)
        sums.append(jnp.sum(s, axis=0, keepdims=True))
    return sums


def grads_kernel(
    first_head,
    is_first,
    query_ref,
    key_ref,
    value_ref,
    dout_ref,
    halo_key_ref,
    halo_value_ref,
    bias_ref,
    dquery_ref,
    dkey_ref,
    dvalue_ref,
    back_key_ref,
    back_value_ref,
    table_ref,
):
    rows, width = query_ref.shape
    heads = width // HEAD_DIM
    scale = HEAD_DIM**-0.5
    lane_head = lax.broadcasted_iota(jnp.int32, (PAIR, width), 1) // HEAD_DIM
    halo_fill = jnp.where(is_first(), NEG_FILL, 0.0)

    def by_head(block):
        zero = jnp.zeros_like(block)
        return jnp.concatenate([jnp.where(lane_head == h, block, zero) for h in range(heads)], axis=0)

    def window(halo_ref, own_ref, start):
        parts = []
        if start < REACH:
            parts.append(halo_ref[start:REACH, :])
        stop = start + WIN - REACH
        parts.append(own_ref[max(start - REACH, 0) : stop, :])
        return jnp.concatenate(parts, axis=0)

    dscore_sum = None
    for pair in range(rows // PAIR):
        start = pair * PAIR
        halo_rows = max(REACH - start, 0)
        query = by_head(query_ref[start : start + PAIR, :])
        dout = by_head(dout_ref[start : start + PAIR, :])
        keys = window(halo_key_ref, key_ref, start)
        values = window(halo_value_ref, value_ref, start)
        scores = dot(keys, query, NT) * scale + bias_ref[...]
        if halo_rows:
            scores = jnp.concatenate([scores[:halo_rows] + halo_fill, scores[halo_rows:]], axis=0)
        peak = jnp.max(scores, axis=0, keepdims=True)
        weights = jnp.exp(scores - peak)
        total = jnp.sum(weights, axis=0, keepdims=True)
        probs = weights * (1.0 / total)
        dprobs = dot(values, dout, NT)
        inner = jnp.sum(probs * dprobs, axis=0, keepdims=True)
        dscores = probs * (dprobs - inner)
        dscore_sum = dscores if dscore_sum is None else dscore_sum + dscores
        prob_half = probs.astype(jnp.bfloat16)
        dscore_half = dscores.astype(jnp.bfloat16)
        dvalue = dot(prob_half, dout, NN)
        dkey = dot(dscore_half, query, NN) * scale
        stacked = dot(dscore_half, keys, TN) * scale
        dquery = stacked[:PAIR]
        for h in range(1, heads):
            dquery = jnp.where(lane_head == h, stacked[h * PAIR : (h + 1) * PAIR], dquery)
        dquery_ref[start : start + PAIR, :] = dquery.astype(jnp.bfloat16)
        if pair == 0:
            back_key_ref[...] = dkey[:REACH].astype(jnp.bfloat16)
            back_value_ref[...] = dvalue[:REACH].astype(jnp.bfloat16)
            held_key = dkey[PAIR:REACH]
            held_value = dvalue[PAIR:REACH]
            dkey_ref[0:PAIR, :] = dkey[REACH:]
            dvalue_ref[0:PAIR, :] = dvalue[REACH:]
        else:
            back_key_ref[PAIR:REACH, :] = (held_key + dkey[:PAIR]).astype(jnp.bfloat16)
            back_value_ref[PAIR:REACH, :] = (held_value + dvalue[:PAIR]).astype(jnp.bfloat16)
            dkey_ref[0:PAIR, :] += dkey[PAIR:REACH]
            dvalue_ref[0:PAIR, :] += dvalue[PAIR:REACH]
            dkey_ref[PAIR:, :] = dkey[REACH:]
            dvalue_ref[PAIR:, :] = dvalue[REACH:]

    key_of = lax.broadcasted_iota(jnp.int32, (PAIR, PAIR), 0)
    query_of = lax.broadcasted_iota(jnp.int32, (PAIR, PAIR), 1)
    after = query_of >= key_of
    squares, tops = [], []
    for h in range(heads):
        lanes = slice(h * PAIR, (h + 1) * PAIR)
        far, middle, near = (dscore_sum[b * PAIR : (b + 1) * PAIR, lanes] for b in range(3))
        squares.append(jnp.where(after, 0.0, near))
        squares.append(jnp.where(after, near, middle))
        tops.append(jnp.sum(far + jnp.where(after, middle, 0.0), axis=0, keepdims=True))
    sums = diagonals(squares)
    last = lax.broadcasted_iota(jnp.int32, (1, PAIR), 1) == PAIR - 1
    pad = [jnp.zeros((8 - heads, PAIR), jnp.float32)]
    neg = jnp.concatenate(sums[0::2] + pad, axis=0)
    pos = jnp.concatenate(
        [s + jnp.where(last, jnp.sum(t, axis=1, keepdims=True), 0.0) for s, t in zip(sums[1::2], tops)] + pad, axis=0
    )
    place = lax.broadcasted_iota(jnp.int32, (8, PAIR), 1) == lax.broadcasted_iota(jnp.int32, (8, PAIR), 0) + first_head(heads)
    place = jnp.where(place & (lax.broadcasted_iota(jnp.int32, (8, PAIR), 0) < heads), 1.0, 0.0)
    table_ref[0:CLIP, :] = dot(neg, place, TN, precision=HIGHEST)
    table_ref[CLIP:, :] = dot(pos, place, TN, precision=HIGHEST)


def first_head(heads):
    return lax.axis_index("tp") * heads


def is_first():
    return lax.axis_index("sp") == 0


def passed_along(block, distance):
    devices = range(lax.axis_size("sp"))
    return lax.ppermute(block, "sp", [(i - distance, i) for i in devices if i - distance in devices])


def shards(query_rows, key_rows, value_rows, out_grad, rel_bias):
    rows, width = query_rows.shape
    heads = width // HEAD_DIM
    table_rows, all_heads = rel_bias.shape
    ranks = lax.axis_size("sp")
    share = table_rows // ranks
    halo_keys = passed_along(key_rows, 1)
    halo_values = passed_along(value_rows, 1)
    bias = pl.pallas_call(
        partial(bias_kernel, first_head),
        out_shape=jax.ShapeDtypeStruct((WIN, heads * PAIR), jnp.float32),
        cost_estimate=pl.CostEstimate(flops=8_000_000_000, bytes_accessed=2_000_000, transcendentals=0),
        compiler_params=pltpu.CompilerParams(vmem_limit_bytes=8 << 20),
        name="bias_tile",
    )(rel_bias)
    half = jax.ShapeDtypeStruct((rows, width), jnp.bfloat16)
    full = jax.ShapeDtypeStruct((rows, width), jnp.float32)
    query_grad, key_own, value_own, back_keys, back_values, table = pl.pallas_call(
        partial(grads_kernel, first_head, is_first),
        out_shape=(half, full, full, half, half, jax.ShapeDtypeStruct((table_rows, PAIR), jnp.float32)),
        cost_estimate=pl.CostEstimate(flops=8_000_000_000, bytes_accessed=4_000_000, transcendentals=0),
        compiler_params=pltpu.CompilerParams(vmem_limit_bytes=24 << 20),
        name="segment_grads",
    )(query_rows, key_rows, value_rows, out_grad, halo_keys, halo_values, bias)
    key_grad = (key_own + passed_along(back_keys, -1)).astype(jnp.bfloat16)
    value_grad = (value_own + passed_along(back_values, -1)).astype(jnp.bfloat16)
    terms = lax.all_to_all(table.reshape(ranks, share, PAIR), "sp", 0, 0, tiled=True)
    mine = jnp.sum(terms, axis=0)
    groups = lax.axis_size("tp")
    copies = lax.all_to_all(jnp.broadcast_to(mine, (groups, share, PAIR)), "tp", 0, 0, tiled=True)
    table_grad = jnp.sum(copies, axis=0)[:, :all_heads]
    return query_grad, key_grad, value_grad, table_grad


def solution(mesh):
    return jax.shard_map(
        shards,
        mesh=mesh,
        in_specs=(P("sp", "tp"), P("sp", "tp"), P("sp", "tp"), P("sp", "tp"), P()),
        out_specs=(P("sp", "tp"), P("sp", "tp"), P("sp", "tp"), P("sp", None)),
        check_vma=False,
    )
```

```python
from functools import partial

import jax
import jax.numpy as jnp
from jax import lax
from jax.experimental import pallas as pl
from jax.experimental.pallas import tpu as pltpu
from jax.sharding import PartitionSpec as P

HEAD_DIM = 64
SEG = 64
LEFT = 4
CLIP = 128
NEG_FILL = -1e30
HIGHEST = lax.Precision.HIGHEST

REACH = LEFT * SEG
PAIR = 2 * SEG
WIN = REACH + PAIR

NT = (((1,), (1,)), ((), ()))
TN = (((0,), (0,)), ((), ()))
NN = (((1,), (0,)), ((), ()))


def dot(a, b, dims, **kw):
    return lax.dot_general(a, b, dims, preferred_element_type=jnp.float32, **kw)


def bias_kernel(first_head, table_ref, bias_ref):
    heads = bias_ref.shape[1] // PAIR
    wide = table_ref.shape[1]
    start = first_head(heads)
    pick = lax.broadcasted_iota(jnp.int32, (8, wide), 1) == lax.broadcasted_iota(jnp.int32, (8, wide), 0) + start
    rows = dot(jnp.where(pick, 1.0, 0.0), table_ref[...], NT, precision=HIGHEST)
    key_of = lax.broadcasted_iota(jnp.int32, (PAIR, PAIR), 0)
    query_of = lax.broadcasted_iota(jnp.int32, (PAIR, PAIR), 1)
    early = query_of < SEG
    low = key_of < SEG
    after = query_of >= key_of
    for head in range(heads):
        lanes = slice(head * PAIR, (head + 1) * PAIR)
        neg = jnp.broadcast_to(rows[head : head + 1, :CLIP], (PAIR, PAIR))
        pos = jnp.broadcast_to(rows[head : head + 1, CLIP:], (PAIR, PAIR))
        neg = pltpu.roll(neg, 0, 1, stride=1, stride_axis=0)
        pos = pltpu.roll(pos, 0, 1, stride=1, stride_axis=0)
        top = rows[head : head + 1, 2 * CLIP - 1 :]
        bias_ref[0:PAIR, lanes] = jnp.where(low & ~early, NEG_FILL, jnp.broadcast_to(top, (PAIR, PAIR)))
        bias_ref[PAIR : 2 * PAIR, lanes] = jnp.where(after, top, pos)
        bias_ref[2 * PAIR : 3 * PAIR, lanes] = jnp.where(early & ~low, NEG_FILL, jnp.where(after, pos, neg))


def diagonals(squares):
    rows = PAIR
    while rows > 8:
        half = rows // 2
        squares = [s[:half] + pltpu.roll(s[half:], PAIR - half, 1) for s in squares]
        rows = half
    row_of = lax.broadcasted_iota(jnp.int32, (8, PAIR), 0)
    sums = []
    for s in squares:
        for bit in (4, 2, 1):
            s = jnp.where((row_of & bit) != 0, pltpu.roll(s, PAIR - bit, 1), s)
        sums.append(jnp.sum(s, axis=0, keepdims=True))
    return sums


def grads_kernel(
    first_head,
    is_first,
    all_heads,
    query_ref,
    key_ref,
    value_ref,
    dout_ref,
    halo_key_ref,
    halo_value_ref,
    bias_ref,
    dquery_ref,
    own_ref,
    back_ref,
    table_ref,
):
    rows, width = query_ref.shape
    heads = width // HEAD_DIM
    scale = HEAD_DIM**-0.5
    lane_head = lax.broadcasted_iota(jnp.int32, (PAIR, width), 1) // HEAD_DIM
    halo_fill = jnp.where(is_first(), NEG_FILL, 0.0)

    def by_head(block):
        zero = jnp.zeros_like(block)
        return jnp.concatenate([jnp.where(lane_head == h, block, zero) for h in range(heads)], axis=0)

    def window(halo_ref, own_ref, start):
        parts = []
        if start < REACH:
            parts.append(halo_ref[start:REACH, :])
        stop = start + WIN - REACH
        parts.append(own_ref[max(start - REACH, 0) : stop, :])
        return jnp.concatenate(parts, axis=0)

    dscore_sum, held = None, []
    for pair in range(rows // PAIR):
        start = pair * PAIR
        halo_rows = max(REACH - start, 0)
        query = by_head(query_ref[start : start + PAIR, :])
        dout = by_head(dout_ref[start : start + PAIR, :])
        keys = window(halo_key_ref, key_ref, start)
        values = window(halo_value_ref, value_ref, start)
        scores = dot(keys, query, NT) * scale + bias_ref[...]
        if halo_rows:
            scores = jnp.concatenate([scores[:halo_rows] + halo_fill, scores[halo_rows:]], axis=0)
        peak = jnp.max(scores, axis=0, keepdims=True)
        weights = jnp.exp(scores - peak)
        total = jnp.sum(weights, axis=0, keepdims=True)
        probs = weights * (1.0 / total)
        dprobs = dot(values, dout, NT)
        inner = jnp.sum(probs * dprobs, axis=0, keepdims=True)
        dscores = probs * (dprobs - inner)
        dscore_sum = dscores if dscore_sum is None else dscore_sum + dscores
        prob_half = probs.astype(jnp.bfloat16)
        dscore_half = dscores.astype(jnp.bfloat16)
        dvalue = dot(prob_half, dout, NN)
        dkey = dot(dscore_half, query, NN) * scale
        stacked = dot(dscore_half, keys, TN) * scale
        dquery = stacked[:PAIR]
        for h in range(1, heads):
            dquery = jnp.where(lane_head == h, stacked[h * PAIR : (h + 1) * PAIR], dquery)
        dquery_ref[start : start + PAIR, :] = dquery.astype(jnp.bfloat16)
        for at, grad in ((0, dkey), (REACH, dvalue)):
            own, back = own_ref.at[at : at + REACH, :], back_ref.at[at : at + REACH, :]
            if pair == 0:
                back[0:PAIR, :] = grad[:PAIR].astype(jnp.bfloat16)
                held.append(grad[PAIR:REACH])
                own[0:PAIR, :] = grad[REACH:]
            else:
                back[PAIR:, :] = (held.pop(0) + grad[:PAIR]).astype(jnp.bfloat16)
                own[0:PAIR, :] += grad[PAIR:REACH]
                own[PAIR:, :] = grad[REACH:]

    key_of = lax.broadcasted_iota(jnp.int32, (PAIR, PAIR), 0)
    query_of = lax.broadcasted_iota(jnp.int32, (PAIR, PAIR), 1)
    after = query_of >= key_of
    squares, tops = [], []
    for h in range(heads):
        lanes = slice(h * PAIR, (h + 1) * PAIR)
        far, middle, near = (dscore_sum[b * PAIR : (b + 1) * PAIR, lanes] for b in range(3))
        squares.append(jnp.where(after, 0.0, near))
        squares.append(jnp.where(after, near, middle))
        tops.append(jnp.sum(far + jnp.where(after, middle, 0.0), axis=0, keepdims=True))
    sums = diagonals(squares)
    last = lax.broadcasted_iota(jnp.int32, (1, PAIR), 1) == PAIR - 1
    pos = [s + jnp.where(last, jnp.sum(t, axis=1, keepdims=True), 0.0) for s, t in zip(sums[1::2], tops)]
    table_ref[...] = by_owner(sums[0::2], pos, table_ref.shape[0], first_head(heads), all_heads)


def by_owner(neg, pos, ranks, start, all_heads):
    share = 2 * CLIP // ranks
    half = ranks // 2
    heads = len(neg)
    mine = lax.broadcasted_iota(jnp.int32, (half, CLIP), 1) // share == lax.broadcasted_iota(jnp.int32, (half, CLIP), 0)
    spread = jnp.concatenate(
        [jnp.concatenate([jnp.where(mine, row, 0.0) for row in rows], axis=1) for rows in (neg, pos)], axis=0
    )
    source = lax.broadcasted_iota(jnp.int32, (heads * CLIP, PAIR), 0)
    lane = lax.broadcasted_iota(jnp.int32, (heads * CLIP, PAIR), 1)
    place = jnp.where(lane == source % share * all_heads + start + source // CLIP, 1.0, 0.0)
    return dot(spread, place, NN, precision=HIGHEST)


def add_kernel(own_ref, arrived_ref, dkey_ref, dvalue_ref):
    rows = dkey_ref.shape[0]
    for at, out_ref in ((0, dkey_ref), (rows, dvalue_ref)):
        total = own_ref[at : at + rows, :] + arrived_ref[at : at + rows, :].astype(jnp.float32)
        out_ref[...] = total.astype(jnp.bfloat16)


def sum_kernel(terms_ref, copies_ref):
    copies_ref[...] = jnp.broadcast_to(jnp.sum(terms_ref[...], axis=0, keepdims=True), copies_ref.shape)


def table_kernel(copies_ref, out_ref):
    row = jnp.sum(copies_ref[...], axis=0, keepdims=True)
    share, heads = out_ref.shape
    for r in range(share):
        out_ref[r : r + 1, :] = row[:, r * heads : (r + 1) * heads]


def first_head(heads):
    return lax.axis_index("tp") * heads


def is_first():
    return lax.axis_index("sp") == 0


def passed_along(block, distance):
    devices = range(lax.axis_size("sp"))
    return lax.ppermute(block, "sp", [(i - distance, i) for i in devices if i - distance in devices])


def shards(query_rows, key_rows, value_rows, out_grad, rel_bias):
    rows, width = query_rows.shape
    heads = width // HEAD_DIM
    table_rows, all_heads = rel_bias.shape
    ranks = lax.axis_size("sp")
    share = table_rows // ranks
    halo_keys = passed_along(key_rows, 1)
    halo_values = passed_along(value_rows, 1)
    bias = pl.pallas_call(
        partial(bias_kernel, first_head),
        out_shape=jax.ShapeDtypeStruct((WIN, heads * PAIR), jnp.float32),
        cost_estimate=pl.CostEstimate(flops=8_000_000_000, bytes_accessed=2_000_000, transcendentals=0),
        compiler_params=pltpu.CompilerParams(vmem_limit_bytes=8 << 20),
        name="bias_tile",
    )(rel_bias)
    half = jax.ShapeDtypeStruct((rows, width), jnp.bfloat16)
    query_grad, own, back, table = pl.pallas_call(
        partial(grads_kernel, first_head, is_first, all_heads),
        out_shape=(
            half,
            jax.ShapeDtypeStruct((2 * rows, width), jnp.float32),
            jax.ShapeDtypeStruct((2 * REACH, width), jnp.bfloat16),
            jax.ShapeDtypeStruct((ranks, PAIR), jnp.float32),
        ),
        cost_estimate=pl.CostEstimate(flops=8_000_000_000, bytes_accessed=4_000_000, transcendentals=0),
        compiler_params=pltpu.CompilerParams(vmem_limit_bytes=24 << 20),
        name="segment_grads",
    )(query_rows, key_rows, value_rows, out_grad, halo_keys, halo_values, bias)
    key_grad, value_grad = pl.pallas_call(
        add_kernel,
        out_shape=(half, half),
        cost_estimate=pl.CostEstimate(flops=1_000_000_000, bytes_accessed=1_000_000, transcendentals=0),
        compiler_params=pltpu.CompilerParams(vmem_limit_bytes=4 << 20),
        name="add_arrived",
    )(own, passed_along(back, -1))
    terms = lax.all_to_all(table.reshape(ranks, 1, PAIR), "sp", 0, 0, tiled=True)
    groups = lax.axis_size("tp")
    copies = pl.pallas_call(
        sum_kernel,
        out_shape=jax.ShapeDtypeStruct((groups, PAIR), jnp.float32),
        compiler_params=pltpu.CompilerParams(vmem_limit_bytes=4 << 20),
        name="sum_of_ranks",
    )(terms.reshape(ranks, PAIR))
    copies = lax.all_to_all(copies.reshape(groups, 1, PAIR), "tp", 0, 0, tiled=True)
    table_grad = pl.pallas_call(
        table_kernel,
        out_shape=jax.ShapeDtypeStruct((share, all_heads), jnp.float32),
        compiler_params=pltpu.CompilerParams(vmem_limit_bytes=4 << 20),
        name="table_rows",
    )(copies.reshape(groups, PAIR))
    return query_grad, key_grad, value_grad, table_grad


def solution(mesh):
    return jax.shard_map(
        shards,
        mesh=mesh,
        in_specs=(P("sp", "tp"), P("sp", "tp"), P("sp", "tp"), P("sp", "tp"), P()),
        out_specs=(P("sp", "tp"), P("sp", "tp"), P("sp", "tp"), P("sp", None)),
        check_vma=False,
    )
```

```python
from functools import partial

import jax
import jax.numpy as jnp
from jax import lax
from jax.experimental import pallas as pl
from jax.experimental.pallas import tpu as pltpu
from jax.sharding import Mesh
from jax.sharding import PartitionSpec as P

HEAD_DIM = 64
SEG = 64
LEFT = 4
CLIP = 128
NEG_FILL = -1e30
SP = ("z", "y")
PLANE = ("y", "tp")
HIGHEST = lax.Precision.HIGHEST

REACH = LEFT * SEG
PAIR = 2 * SEG
WIN = REACH + PAIR

NT = (((1,), (1,)), ((), ()))
TN = (((0,), (0,)), ((), ()))
NN = (((1,), (0,)), ((), ()))


def dot(a, b, dims, **kw):
    return lax.dot_general(a, b, dims, preferred_element_type=jnp.float32, **kw)


def bias_kernel(first_head, table_ref, bias_ref):
    heads = bias_ref.shape[1] // PAIR
    wide = table_ref.shape[1]
    start = first_head(heads)
    pick = lax.broadcasted_iota(jnp.int32, (8, wide), 1) == lax.broadcasted_iota(jnp.int32, (8, wide), 0) + start
    rows = dot(jnp.where(pick, 1.0, 0.0), table_ref[...], NT, precision=HIGHEST)
    key_of = lax.broadcasted_iota(jnp.int32, (PAIR, PAIR), 0)
    query_of = lax.broadcasted_iota(jnp.int32, (PAIR, PAIR), 1)
    early = query_of < SEG
    low = key_of < SEG
    after = query_of >= key_of
    for head in range(heads):
        lanes = slice(head * PAIR, (head + 1) * PAIR)
        neg = jnp.broadcast_to(rows[head : head + 1, :CLIP], (PAIR, PAIR))
        pos = jnp.broadcast_to(rows[head : head + 1, CLIP:], (PAIR, PAIR))
        neg = pltpu.roll(neg, 0, 1, stride=1, stride_axis=0)
        pos = pltpu.roll(pos, 0, 1, stride=1, stride_axis=0)
        top = rows[head : head + 1, 2 * CLIP - 1 :]
        bias_ref[0:PAIR, lanes] = jnp.where(low & ~early, NEG_FILL, jnp.broadcast_to(top, (PAIR, PAIR)))
        bias_ref[PAIR : 2 * PAIR, lanes] = jnp.where(after, top, pos)
        bias_ref[2 * PAIR : 3 * PAIR, lanes] = jnp.where(early & ~low, NEG_FILL, jnp.where(after, pos, neg))


def diagonals(squares):
    rows = PAIR
    while rows > 8:
        half = rows // 2
        squares = [s[:half] + pltpu.roll(s[half:], PAIR - half, 1) for s in squares]
        rows = half
    row_of = lax.broadcasted_iota(jnp.int32, (8, PAIR), 0)
    sums = []
    for s in squares:
        for bit in (4, 2, 1):
            s = jnp.where((row_of & bit) != 0, pltpu.roll(s, PAIR - bit, 1), s)
        sums.append(jnp.sum(s, axis=0, keepdims=True))
    return sums


def by_head(block, width):
    lane_head = lax.broadcasted_iota(jnp.int32, block.shape, 1) // HEAD_DIM
    zero = jnp.zeros_like(block)
    return jnp.concatenate([jnp.where(lane_head == h, block, zero) for h in range(width // HEAD_DIM)], axis=0)


def window(halo_ref, own_ref, pair):
    start = pair * PAIR
    parts = [halo_ref[start:REACH, :]] if start < REACH else []
    parts.append(own_ref[max(start - REACH, 0) : start + PAIR, :])
    return jnp.concatenate(parts, axis=0)


def probs_kernel(is_first, query_ref, key_ref, halo_ref, bias_ref, probs_ref, half_ref):
    rows, width = query_ref.shape
    halo_fill = jnp.where(is_first(), NEG_FILL, 0.0)
    for pair in range(rows // PAIR):
        start = pair * PAIR
        halo_rows = max(REACH - start, 0)
        query = by_head(query_ref[start : start + PAIR, :], width)
        scores = dot(window(halo_ref, key_ref, pair), query, NT) * HEAD_DIM**-0.5 + bias_ref[...]
        if halo_rows:
            scores = jnp.concatenate([scores[:halo_rows] + halo_fill, scores[halo_rows:]], axis=0)
        peak = jnp.max(scores, axis=0, keepdims=True)
        weights = jnp.exp(scores - peak)
        total = jnp.sum(weights, axis=0, keepdims=True)
        probs = weights * (1.0 / total)
        probs_ref[pair * WIN : (pair + 1) * WIN, :] = probs
        half_ref[pair * WIN : (pair + 1) * WIN, :] = probs.astype(jnp.bfloat16)


def dscores_kernel(value_ref, dout_ref, halo_ref, probs_ref, dscores_ref, table_ref):
    rows, width = value_ref.shape
    heads = width // HEAD_DIM
    dscore_sum = None
    for pair in range(rows // PAIR):
        start = pair * PAIR
        dout = by_head(dout_ref[start : start + PAIR, :], width)
        dprobs = dot(window(halo_ref, value_ref, pair), dout, NT)
        probs = probs_ref[pair * WIN : (pair + 1) * WIN, :]
        inner = jnp.sum(probs * dprobs, axis=0, keepdims=True)
        dscores = probs * (dprobs - inner)
        dscore_sum = dscores if dscore_sum is None else dscore_sum + dscores
        dscores_ref[pair * WIN : (pair + 1) * WIN, :] = dscores.astype(jnp.bfloat16)
    key_of = lax.broadcasted_iota(jnp.int32, (PAIR, PAIR), 0)
    query_of = lax.broadcasted_iota(jnp.int32, (PAIR, PAIR), 1)
    after = query_of >= key_of
    squares, tops = [], []
    for h in range(heads):
        lanes = slice(h * PAIR, (h + 1) * PAIR)
        far, middle, near = (dscore_sum[b * PAIR : (b + 1) * PAIR, lanes] for b in range(3))
        squares.append(jnp.where(after, 0.0, near))
        squares.append(jnp.where(after, near, middle))
        tops.append(jnp.sum(far + jnp.where(after, middle, 0.0), axis=0, keepdims=True))
    sums = diagonals(squares)
    last = lax.broadcasted_iota(jnp.int32, (1, PAIR), 1) == PAIR - 1
    pos = [s + jnp.where(last, jnp.sum(t, axis=1, keepdims=True), 0.0) for s, t in zip(sums[1::2], tops)]
    by_rank = by_owner(sums[0::2], pos)
    ranks = lax.axis_size("y")
    share = by_rank.shape[0] // ranks
    copies = table_ref.shape[0] // by_rank.shape[0]
    for y in range(ranks):
        block = jnp.concatenate([by_rank[y * share : (y + 1) * share, :]] * copies, axis=0)
        table_ref[y * share * copies : (y + 1) * share * copies, :] = block


def by_owner(neg, pos):
    heads = len(neg)
    period = 2 * CLIP // lax.axis_size("z")
    rows = lax.broadcasted_iota(jnp.int32, (period, CLIP), 0)
    mine = lax.broadcasted_iota(jnp.int32, (period, CLIP), 1) % period == rows
    spread = jnp.concatenate([jnp.where(mine, row, 0.0) for row in neg + pos], axis=1)
    source = lax.broadcasted_iota(jnp.int32, (2 * heads * CLIP, PAIR), 0)
    lane = lax.broadcasted_iota(jnp.int32, (2 * heads * CLIP, PAIR), 1)
    head = source // CLIP % heads
    index = source % CLIP + source // (heads * CLIP) * CLIP
    place = jnp.where(lane == index // period * heads + head, 1.0, 0.0)
    return dot(spread, place, NN, precision=HIGHEST)


def heads_kernel(heads, all_heads, terms_ref, out_ref):
    ranks, groups = lax.axis_size("z"), lax.axis_size("tp")
    share = 2 * CLIP // lax.axis_size(SP)
    each = groups * share
    total = terms_ref[0:each, :]
    for y in range(1, lax.axis_size("y")):
        total = total + terms_ref[y * each : (y + 1) * each, :]
    source = lax.broadcasted_iota(jnp.int32, (each, PAIR), 0)
    lane = lax.broadcasted_iota(jnp.int32, (each, PAIR), 1)
    wanted = (lane // all_heads == source % share) & (lane % all_heads // heads == source // share)
    spread = dot(total, jnp.where(wanted, 1.0, 0.0), TN, precision=HIGHEST)
    source = lax.broadcasted_iota(jnp.int32, (PAIR, PAIR), 0)
    lane = lax.broadcasted_iota(jnp.int32, (PAIR, PAIR), 1)
    spread = jnp.where(source % heads == lane % heads, spread, 0.0)
    rank = (lax.broadcasted_iota(jnp.int32, (ranks, PAIR), 0) + ranks // 2) % ranks
    pick = lax.broadcasted_iota(jnp.int32, (ranks, PAIR), 1) // heads == rank
    out_ref[...] = dot(jnp.where(pick, 1.0, 0.0), spread, NN, precision=HIGHEST)


def grads_kernel(
    query_ref, key_ref, dout_ref, halo_ref, probs_ref, dscores_ref, dquery_ref, own_ref, back_ref
):
    rows, width = query_ref.shape
    heads = width // HEAD_DIM
    scale = HEAD_DIM**-0.5
    lane_head = lax.broadcasted_iota(jnp.int32, (PAIR, width), 1) // HEAD_DIM
    held = []
    for pair in range(rows // PAIR):
        start = pair * PAIR
        query = by_head(query_ref[start : start + PAIR, :], width)
        dout = by_head(dout_ref[start : start + PAIR, :], width)
        prob_half = probs_ref[pair * WIN : (pair + 1) * WIN, :]
        dscore_half = dscores_ref[pair * WIN : (pair + 1) * WIN, :]
        dvalue = dot(prob_half, dout, NN)
        dkey = dot(dscore_half, query, NN) * scale
        stacked = dot(dscore_half, window(halo_ref, key_ref, pair), TN) * scale
        dquery = stacked[:PAIR]
        for h in range(1, heads):
            dquery = jnp.where(lane_head == h, stacked[h * PAIR : (h + 1) * PAIR], dquery)
        dquery_ref[start : start + PAIR, :] = dquery.astype(jnp.bfloat16)
        for at, grad in ((0, dkey), (REACH, dvalue)):
            own, back = own_ref.at[at : at + REACH, :], back_ref.at[at : at + REACH, :]
            if pair == 0:
                back[0:PAIR, :] = grad[:PAIR].astype(jnp.bfloat16)
                held.append(grad[PAIR:REACH])
                own[0:PAIR, :] = grad[REACH:]
            else:
                back[PAIR:, :] = (held.pop(0) + grad[:PAIR]).astype(jnp.bfloat16)
                own[0:PAIR, :] += grad[PAIR:REACH]
                own[PAIR:, :] = grad[REACH:]


def last_kernel(own_ref, arrived_ref, terms_ref, dkey_ref, dvalue_ref, table_ref):
    rows = dkey_ref.shape[0]
    for at, out_ref in ((0, dkey_ref), (rows, dvalue_ref)):
        total = own_ref[at : at + rows, :] + arrived_ref[at : at + rows, :].astype(jnp.float32)
        out_ref[...] = total.astype(jnp.bfloat16)
    row = jnp.sum(terms_ref[...], axis=0, keepdims=True)
    share, heads = table_ref.shape
    for r in range(share):
        table_ref[r : r + 1, :] = row[:, r * heads : (r + 1) * heads]


def first_head(heads):
    return lax.axis_index("tp") * heads


def is_first():
    return lax.axis_index(SP) == 0


def passed_along(block, distance):
    devices = range(lax.axis_size(SP))
    return lax.ppermute(block, SP, [(i - distance, i) for i in devices if i - distance in devices])


def kernel(body, outs, flops):
    return pl.pallas_call(
        body,
        out_shape=outs,
        cost_estimate=pl.CostEstimate(flops=flops, bytes_accessed=2_000_000, transcendentals=0),
        compiler_params=pltpu.CompilerParams(vmem_limit_bytes=16 << 20),
    )


def shards(query_rows, key_rows, value_rows, out_grad, rel_bias):
    rows, width = query_rows.shape
    heads = width // HEAD_DIM
    all_heads = rel_bias.shape[1]
    ranks, groups = lax.axis_size("z"), lax.axis_size(PLANE)
    share = 2 * CLIP // lax.axis_size(SP)
    pairs = rows // PAIR
    struct = jax.ShapeDtypeStruct
    half = struct((rows, width), jnp.bfloat16)
    wide = struct((pairs * WIN, heads * PAIR), jnp.float32)
    wide_half = struct(wide.shape, jnp.bfloat16)

    halo_keys = passed_along(key_rows, 1)
    halo_values = passed_along(value_rows, 1)
    bias_shape = struct((WIN, heads * PAIR), jnp.float32)
    bias = kernel(partial(bias_kernel, first_head), bias_shape, 2_000_000_000)(rel_bias)
    probs, prob_half = kernel(partial(probs_kernel, is_first), (wide, wide_half), 4_000_000_000)(
        query_rows, key_rows, halo_keys, bias
    )
    outs = (wide_half, struct((groups * share, PAIR), jnp.float32))
    dscores, table = kernel(dscores_kernel, outs, 4_000_000_000)(value_rows, out_grad, halo_values, probs)
    terms = lax.all_to_all(table.reshape(groups, share, PAIR), PLANE, 0, 0, tiled=True)
    outs = (half, struct((2 * rows, width), jnp.float32), struct((2 * REACH, width), jnp.bfloat16))
    query_grad, own, back = kernel(grads_kernel, outs, 4_000_000_000)(
        query_rows, key_rows, out_grad, halo_keys, prob_half, dscores
    )
    arrived = passed_along(back, -1)
    table = kernel(
        partial(heads_kernel, heads, all_heads), struct((ranks, PAIR), jnp.float32), 500_000_000
    )(terms.reshape(groups * share, PAIR))
    order = [[(i + ranks // 2) % ranks for i in range(ranks)]]
    terms = lax.all_to_all(table.reshape(ranks, 1, PAIR), "z", 0, 0, axis_index_groups=order, tiled=True)
    outs = (half, half, struct((share, all_heads), jnp.float32))
    key_grad, value_grad, table_grad = kernel(last_kernel, outs, 500_000_000)(own, arrived, terms.reshape(ranks, PAIR))
    return query_grad, key_grad, value_grad, table_grad


def solution(mesh):
    finer = Mesh(mesh.devices.reshape(-1, 4, mesh.shape["tp"]), ("z", "y", "tp"))
    return jax.shard_map(
        shards,
        mesh=finer,
        in_specs=(P(SP, "tp"), P(SP, "tp"), P(SP, "tp"), P(SP, "tp"), P()),
        out_specs=(P(SP, "tp"), P(SP, "tp"), P(SP, "tp"), P(SP, None)),
        check_vma=False,
    )
```

```python
from functools import partial

import jax
import jax.numpy as jnp
from jax import lax
from jax.experimental import pallas as pl
from jax.experimental.pallas import tpu as pltpu
from jax.sharding import Mesh
from jax.sharding import PartitionSpec as P

HEAD_DIM = 64
SEG = 64
LEFT = 4
CLIP = 128
NEG_FILL = -1e30
SP = ("z", "y")
PLANE = ("y", "tp")
HIGHEST = lax.Precision.HIGHEST

REACH = LEFT * SEG
PAIR = 2 * SEG
WIN = REACH + PAIR

NT = (((1,), (1,)), ((), ()))
TN = (((0,), (0,)), ((), ()))
NN = (((1,), (0,)), ((), ()))


def dot(a, b, dims, **kw):
    return lax.dot_general(a, b, dims, preferred_element_type=jnp.float32, **kw)


def bias_kernel(first_head, table_ref, bias_ref):
    heads = bias_ref.shape[1] // PAIR
    wide = table_ref.shape[1]
    start = first_head(heads)
    pick = lax.broadcasted_iota(jnp.int32, (8, wide), 1) == lax.broadcasted_iota(jnp.int32, (8, wide), 0) + start
    rows = dot(jnp.where(pick, 1.0, 0.0), table_ref[...], NT, precision=HIGHEST)
    key_of = lax.broadcasted_iota(jnp.int32, (PAIR, PAIR), 0)
    query_of = lax.broadcasted_iota(jnp.int32, (PAIR, PAIR), 1)
    early = query_of < SEG
    low = key_of < SEG
    after = query_of >= key_of
    for head in range(heads):
        lanes = slice(head * PAIR, (head + 1) * PAIR)
        neg = jnp.broadcast_to(rows[head : head + 1, :CLIP], (PAIR, PAIR))
        pos = jnp.broadcast_to(rows[head : head + 1, CLIP:], (PAIR, PAIR))
        neg = pltpu.roll(neg, 0, 1, stride=1, stride_axis=0)
        pos = pltpu.roll(pos, 0, 1, stride=1, stride_axis=0)
        top = rows[head : head + 1, 2 * CLIP - 1 :]
        bias_ref[0:PAIR, lanes] = jnp.where(low & ~early, NEG_FILL, jnp.broadcast_to(top, (PAIR, PAIR)))
        bias_ref[PAIR : 2 * PAIR, lanes] = jnp.where(after, top, pos)
        bias_ref[2 * PAIR : 3 * PAIR, lanes] = jnp.where(early & ~low, NEG_FILL, jnp.where(after, pos, neg))


def diagonals(squares):
    rows = PAIR
    while rows > 8:
        half = rows // 2
        squares = [s[:half] + pltpu.roll(s[half:], PAIR - half, 1) for s in squares]
        rows = half
    row_of = lax.broadcasted_iota(jnp.int32, (8, PAIR), 0)
    sums = []
    for s in squares:
        for bit in (4, 2, 1):
            s = jnp.where((row_of & bit) != 0, pltpu.roll(s, PAIR - bit, 1), s)
        sums.append(jnp.sum(s, axis=0, keepdims=True))
    return sums


def by_head(block, width):
    lane_head = lax.broadcasted_iota(jnp.int32, block.shape, 1) // HEAD_DIM
    zero = jnp.zeros_like(block)
    return jnp.concatenate([jnp.where(lane_head == h, block, zero) for h in range(width // HEAD_DIM)], axis=0)


def window(halo_ref, own_ref, pair):
    start = pair * PAIR
    parts = [halo_ref[start:REACH, :]] if start < REACH else []
    parts.append(own_ref[max(start - REACH, 0) : start + PAIR, :])
    return jnp.concatenate(parts, axis=0)


def probs_kernel(is_first, query_ref, key_ref, halo_ref, bias_ref, probs_ref, half_ref):
    rows, width = query_ref.shape
    halo_fill = jnp.where(is_first(), NEG_FILL, 0.0)
    for pair in range(rows // PAIR):
        start = pair * PAIR
        halo_rows = max(REACH - start, 0)
        query = by_head(query_ref[start : start + PAIR, :], width)
        scores = dot(window(halo_ref, key_ref, pair), query, NT) * HEAD_DIM**-0.5 + bias_ref[...]
        if halo_rows:
            scores = jnp.concatenate([scores[:halo_rows] + halo_fill, scores[halo_rows:]], axis=0)
        peak = jnp.max(scores, axis=0, keepdims=True)
        weights = jnp.exp(scores - peak)
        total = jnp.sum(weights, axis=0, keepdims=True)
        probs = weights * (1.0 / total)
        probs_ref[pair * WIN : (pair + 1) * WIN, :] = probs
        half_ref[pair * WIN : (pair + 1) * WIN, :] = probs.astype(jnp.bfloat16)


def thirds(block):
    high = block.astype(jnp.bfloat16)
    rest = block - high.astype(jnp.float32)
    middle = rest.astype(jnp.bfloat16)
    return high, middle, (rest - middle.astype(jnp.float32)).astype(jnp.bfloat16)


def dscores_kernel(value_ref, dout_ref, halo_ref, probs_ref, dscores_ref, table_ref):
    rows, width = value_ref.shape
    heads = width // HEAD_DIM
    pairs = rows // PAIR
    key_of = lax.broadcasted_iota(jnp.int32, (PAIR, PAIR), 0)
    query_of = lax.broadcasted_iota(jnp.int32, (PAIR, PAIR), 1)
    after = query_of >= key_of
    last = lax.broadcasted_iota(jnp.int32, (1, PAIR), 1) == PAIR - 1
    douts = [by_head(dout_ref[p * PAIR : (p + 1) * PAIR, :], width) for p in range(pairs)]
    values = [window(halo_ref, value_ref, p) for p in range(pairs)]
    neg, pos = [], []
    for first in range(0, heads, 2):
        dprobs = [dot(values[p], douts[p][first * PAIR : (first + 2) * PAIR], NT) for p in range(pairs)]
        for head in (first, first + 1):
            lanes = slice(head * PAIR, (head + 1) * PAIR)
            mine = [d[:, (head - first) * PAIR : (head - first + 1) * PAIR] for d in dprobs]
            inner = [
                jnp.sum(probs_ref[p * WIN : (p + 1) * WIN, lanes] * mine[p], axis=0, keepdims=True) for p in range(pairs)
            ]
            blocks = []
            for b in range(WIN // PAIR):
                total = None
                for p in range(pairs):
                    at = slice(p * WIN + b * PAIR, p * WIN + (b + 1) * PAIR)
                    dscores = probs_ref[at, lanes] * (mine[p][b * PAIR : (b + 1) * PAIR] - inner[p])
                    dscores_ref[at, lanes] = dscores.astype(jnp.bfloat16)
                    total = dscores if total is None else total + dscores
                blocks.append(total)
            far, middle, near = blocks
            top = jnp.sum(far + jnp.where(after, middle, 0.0), axis=0, keepdims=True)
            below, above = diagonals([jnp.where(after, 0.0, near), jnp.where(after, near, middle)])
            neg.append(below)
            pos.append(above + jnp.where(last, jnp.sum(top, axis=1, keepdims=True), 0.0))
    by_rank = by_owner([jnp.concatenate([n, p], axis=1) for n, p in zip(neg, pos)])
    ranks = lax.axis_size("y")
    share = by_rank.shape[0] // ranks
    copies = table_ref.shape[0] // by_rank.shape[0]
    for y in range(ranks):
        block = jnp.concatenate([by_rank[y * share : (y + 1) * share, :]] * copies, axis=0)
        table_ref[y * share * copies : (y + 1) * share * copies, :] = block


def by_owner(columns):
    heads, table_rows = len(columns), 2 * CLIP
    period = table_rows // lax.axis_size("z")
    iota = partial(lax.broadcasted_iota, jnp.int32)
    mine = iota((period, table_rows), 1) % period == iota((period, table_rows), 0)
    spread = jnp.concatenate([jnp.where(mine, column, 0.0) for column in columns], axis=0)
    rank = iota((table_rows, PAIR), 0) // period
    place = jnp.where(iota((table_rows, PAIR), 1) // heads == rank, 1.0, 0.0).astype(jnp.bfloat16)
    count = heads * period
    found = dot(jnp.concatenate(thirds(spread), axis=0), place, NN)
    found = found[:count] + found[count : 2 * count] + found[2 * count :]
    head_of = iota((period, PAIR), 1) % heads
    out = found[:period]
    for h in range(1, heads):
        out = jnp.where(head_of == h, found[h * period : (h + 1) * period], out)
    return out


def heads_kernel(heads, all_heads, terms_ref, out_ref):
    ranks, groups = lax.axis_size("z"), lax.axis_size("tp")
    share = 2 * CLIP // lax.axis_size(SP)
    each = groups * share
    total = terms_ref[0:each, :]
    for y in range(1, lax.axis_size("y")):
        total = total + terms_ref[y * each : (y + 1) * each, :]
    iota = partial(lax.broadcasted_iota, jnp.int32)
    source, lane = iota((each, PAIR), 0), iota((each, PAIR), 1)
    wanted = (lane // all_heads == source % share) & (lane % all_heads // heads == source // share)
    place = jnp.where(wanted, 1.0, 0.0).astype(jnp.bfloat16)
    spread = dot(jnp.concatenate(thirds(total), axis=0), jnp.concatenate([place] * 3, axis=0), TN)
    spread = jnp.where(iota((PAIR, PAIR), 0) % heads == iota((PAIR, PAIR), 1) % heads, spread, 0.0)
    rank = (iota((ranks, PAIR), 0) + ranks // 2) % ranks
    pick = jnp.where(iota((ranks, PAIR), 1) // heads == rank, 1.0, 0.0).astype(jnp.bfloat16)
    out_ref[...] = dot(jnp.concatenate([pick] * 3, axis=1), jnp.concatenate(thirds(spread), axis=0), NN)


def grads_kernel(
    query_ref, key_ref, dout_ref, halo_ref, probs_ref, dscores_ref, dquery_ref, own_ref, back_ref
):
    rows, width = query_ref.shape
    heads = width // HEAD_DIM
    scale = HEAD_DIM**-0.5
    lane_head = lax.broadcasted_iota(jnp.int32, (PAIR, width), 1) // HEAD_DIM
    held = []
    for pair in range(rows // PAIR):
        start = pair * PAIR
        query = by_head(query_ref[start : start + PAIR, :], width)
        dout = by_head(dout_ref[start : start + PAIR, :], width)
        prob_half = probs_ref[pair * WIN : (pair + 1) * WIN, :]
        dscore_half = dscores_ref[pair * WIN : (pair + 1) * WIN, :]
        dvalue = dot(prob_half, dout, NN)
        dkey = dot(dscore_half, query, NN) * scale
        stacked = dot(dscore_half, window(halo_ref, key_ref, pair), TN) * scale
        dquery = stacked[:PAIR]
        for h in range(1, heads):
            dquery = jnp.where(lane_head == h, stacked[h * PAIR : (h + 1) * PAIR], dquery)
        dquery_ref[start : start + PAIR, :] = dquery.astype(jnp.bfloat16)
        for at, grad in ((0, dkey), (REACH, dvalue)):
            own, back = own_ref.at[at : at + REACH, :], back_ref.at[at : at + REACH, :]
            if pair == 0:
                back[0:PAIR, :] = grad[:PAIR].astype(jnp.bfloat16)
                held.append(grad[PAIR:REACH])
                own[0:PAIR, :] = grad[REACH:]
            else:
                back[PAIR:, :] = (held.pop(0) + grad[:PAIR]).astype(jnp.bfloat16)
                own[0:PAIR, :] += grad[PAIR:REACH]
                own[PAIR:, :] = grad[REACH:]


def last_kernel(own_ref, arrived_ref, terms_ref, dkey_ref, dvalue_ref, table_ref):
    rows = dkey_ref.shape[0]
    for at, out_ref in ((0, dkey_ref), (rows, dvalue_ref)):
        total = own_ref[at : at + rows, :] + arrived_ref[at : at + rows, :].astype(jnp.float32)
        out_ref[...] = total.astype(jnp.bfloat16)
    row = jnp.sum(terms_ref[...], axis=0, keepdims=True)
    share, heads = table_ref.shape
    for r in range(share):
        table_ref[r : r + 1, :] = row[:, r * heads : (r + 1) * heads]


def first_head(heads):
    return lax.axis_index("tp") * heads


def is_first():
    return lax.axis_index(SP) == 0


def passed_along(block, distance):
    devices = range(lax.axis_size(SP))
    return lax.ppermute(block, SP, [(i - distance, i) for i in devices if i - distance in devices])


def kernel(body, outs, flops):
    return pl.pallas_call(
        body,
        out_shape=outs,
        cost_estimate=pl.CostEstimate(flops=flops, bytes_accessed=2_000_000, transcendentals=0),
        compiler_params=pltpu.CompilerParams(vmem_limit_bytes=16 << 20),
    )


def shards(query_rows, key_rows, value_rows, out_grad, rel_bias):
    rows, width = query_rows.shape
    heads = width // HEAD_DIM
    all_heads = rel_bias.shape[1]
    ranks, groups = lax.axis_size("z"), lax.axis_size(PLANE)
    share = 2 * CLIP // lax.axis_size(SP)
    pairs = rows // PAIR
    struct = jax.ShapeDtypeStruct
    half = struct((rows, width), jnp.bfloat16)
    wide = struct((pairs * WIN, heads * PAIR), jnp.float32)
    wide_half = struct(wide.shape, jnp.bfloat16)

    halo_keys = passed_along(key_rows, 1)
    halo_values = passed_along(value_rows, 1)
    bias_shape = struct((WIN, heads * PAIR), jnp.float32)
    bias = kernel(partial(bias_kernel, first_head), bias_shape, 2_000_000_000)(rel_bias)
    probs, prob_half = kernel(partial(probs_kernel, is_first), (wide, wide_half), 4_000_000_000)(
        query_rows, key_rows, halo_keys, bias
    )
    outs = (wide_half, struct((groups * share, PAIR), jnp.float32))
    dscores, table = kernel(dscores_kernel, outs, 4_000_000_000)(value_rows, out_grad, halo_values, probs)
    terms = lax.all_to_all(table.reshape(groups, share, PAIR), PLANE, 0, 0, tiled=True)
    outs = (half, struct((2 * rows, width), jnp.float32), struct((2 * REACH, width), jnp.bfloat16))
    query_grad, own, back = kernel(grads_kernel, outs, 4_000_000_000)(
        query_rows, key_rows, out_grad, halo_keys, prob_half, dscores
    )
    arrived = passed_along(back, -1)
    table = kernel(
        partial(heads_kernel, heads, all_heads), struct((ranks, PAIR), jnp.float32), 500_000_000
    )(terms.reshape(groups * share, PAIR))
    order = [[(i + ranks // 2) % ranks for i in range(ranks)]]
    terms = lax.all_to_all(table.reshape(ranks, 1, PAIR), "z", 0, 0, axis_index_groups=order, tiled=True)
    outs = (half, half, struct((share, all_heads), jnp.float32))
    key_grad, value_grad, table_grad = kernel(last_kernel, outs, 500_000_000)(own, arrived, terms.reshape(ranks, PAIR))
    return query_grad, key_grad, value_grad, table_grad


def solution(mesh):
    finer = Mesh(mesh.devices.reshape(-1, 4, mesh.shape["tp"]), ("z", "y", "tp"))
    return jax.shard_map(
        shards,
        mesh=finer,
        in_specs=(P(SP, "tp"), P(SP, "tp"), P(SP, "tp"), P(SP, "tp"), P()),
        out_specs=(P(SP, "tp"), P(SP, "tp"), P(SP, "tp"), P(SP, None)),
        check_vma=False,
    )
```
